32 devices in a mesh: gr: 2 (over x), fs: 8 (over z, y), tp: 2 (over core).
Axes of the slice: x: 2, y: 2, z: 4, core: 2. Of those that a mesh axis runs over, the one named last changes fastest.
Arguments:
- tokens: bfloat16 [4096, 2048], P(('gr', 'fs')), may hold values from -6 to 6
- norm_gain: float32 [2048], P(('gr', 'fs')), may hold values from 0.1 to 1.9
- gate_train: float32 [8, 2048, 1024], P(None, ('gr', 'fs'), 'tp'), may hold values from -0.125 to 0.125
- up_train: float32 [8, 2048, 1024], P(None, ('gr', 'fs'), 'tp'), may hold values from -0.125 to 0.125
- down_train: float32 [8, 1024, 2048], P(None, 'tp', ('gr', 'fs')), may hold values from -0.1875 to 0.1875
- expert_ids: int32 [4096, 2], P(('gr', 'fs')), may hold values from 0 to 7, all different within a row; in each aligned block of 256 rows (0 to 255, 256 to 511, ...) at most 128 rows name the same one
- route_score: float32 [4096, 2], P(('gr', 'fs')), may hold values from 0.05 to 1
Outputs:
- gate_ready: bfloat16 [8, 2048, 1024], P('fs', None, 'tp')
- up_ready: bfloat16 [8, 2048, 1024], P('fs', None, 'tp')
- down_ready: bfloat16 [8, 1024, 2048], P('fs', 'tp')
- mixed: bfloat16 [4096, 2048], P(('gr', 'fs'), 'tp')
The draws below stay inside these ranges and needn't reach their ends.
Inputs may be any that keep to these rules, and one draw needn't show every extreme that they name: `expert_ids`: each row names two different experts. Among the 256 rows of one device no expert is named more than 128 times, and in every draw some expert is named exactly 128 times by some device's rows.
All inputs are finite; a program needn't handle non-finite values.
Results may differ from the reference program's by a relative error of at most 0.015.
Values may be sent and summed in bfloat16 or wider, within the bound.
A program may use at most 64 MiB of HBM per device.

```python
import math
import jax
import jax.numpy as jnp
import numpy as np
from jax import lax

D = 2048
FF = 1024
TOK_DEV = 256
EXPERTS = 8
CAP = 128
TOKENS = 4096
N_GR = 2
N_FS = 8
N_TP = 2


def block_levels(stream_key, dims, pieces, least, top_value):
    loudness, own = 1.0, jax.random.fold_in(stream_key, 6)
    for dim, parts in pieces:
        draws = jnp.exp(jax.random.uniform(jax.random.fold_in(own, dim), (parts,), jnp.float32, least / len(pieces), top_value / len(pieces)))
        loudness = loudness * jnp.repeat(draws, dims[dim] // parts).reshape([-1 if axis == dim else 1 for axis in range(len(dims))])
    return loudness


def assign_block(own_key, own, number, rows, count, top, most, slope):
    ranking = jax.random.permutation(own_key, count)
    crowded, usual = portions_of(count, rows * top, most, slope, True), portions_of(count, rows * top, most, slope, False)
    places = jnp.arange(count)

    def named(lengths, rotation):
        used = int((lengths > 0).sum())
        fixed = max(1, used // 4)
        moved = fixed + (places - fixed + rotation * (used - fixed)) % max(1, count - fixed)
        return jnp.zeros((count,), jnp.int32).at[ranking[jnp.where(places < fixed, places, moved)]].set(jnp.asarray(lengths, jnp.int32))

    lengths = jnp.where(number % 4 == 0, named(crowded, number // 4), named(usual, number - number // 4 - 1))
    mixed = jax.random.permutation(jax.random.fold_in(own, 3), count)
    source_of, receiver = mixed[0:count // 2 * 2:2], mixed[1:count // 2 * 2:2]
    slack = jnp.minimum(lengths[source_of] - 1, most - lengths[receiver]) // 2
    slack = jnp.where((source_of == ranking[0]) | (receiver == ranking[0]) | (lengths[receiver] == 0), 0, jnp.maximum(slack, 0))
    moved = jax.random.randint(jax.random.fold_in(own, 4), (count // 2,), 0, 1 << 20) % (slack + 1)
    lengths = lengths.at[source_of].add(-moved).at[receiver].add(moved)
    members = jnp.searchsorted(jnp.cumsum(lengths), jnp.arange(rows * top), side="right").astype(jnp.int32)
    table = members.reshape(top, rows).T
    table = table[jax.random.permutation(jax.random.fold_in(own, 1), rows)]
    rotation = jax.random.randint(jax.random.fold_in(own, 2), (rows, 1), 0, top)
    return jnp.take_along_axis(table, (jnp.arange(top)[None, :] + rotation) % top, axis=1)


def portions_of(amount, total, reach, slope, full):
    portions = [(1 << 20) // math.isqrt(standing ** slope) + 1 for standing in range(1, amount + 1)]
    largest = reach if full else min(reach, max(-(-total // amount), total * portions[0] // sum(portions)))
    least = 1 if total - largest >= amount - 1 else 0
    holding, rest = [largest] + [least] * (amount - 1), total - largest - least * (amount - 1)
    while rest > 0:
        candidates = [i for i in range(1, amount) if holding[i] < largest] or [i for i in range(1, amount) if holding[i] < reach]
        pool, left = sum([portions[i] for i in candidates]), rest
        for i in candidates:
            addition = min(reach - holding[i], max(1, left * portions[i] // pool), rest)
            holding[i] = holding[i] + addition
            rest = rest - addition
    return np.array(holding)


def gaussian(own_key, shape, scale, bound, split=(), kind=jnp.bfloat16):
    result = scale * jax.random.normal(own_key, shape, jnp.float32)
    if split:
        result = result * block_levels(own_key, shape, split, -0.22, 0.18)
    return jnp.clip(result, -bound, bound).astype(kind)


def setup_inputs(seed: int = 0) -> dict:
    key_list = jax.random.split(jax.random.key(seed), 8)
    tokens = gaussian(key_list[0], (TOKENS, D), 1.0, 6.0, ((0, 16),))
    norm_gain = jnp.clip(1.0 + 0.18 * jax.random.normal(key_list[1], (D,), jnp.float32), 0.1, 1.9)
    gate_train = gaussian(key_list[2], (EXPERTS, D, FF), D ** -0.5, 0.125, ((1, 16), (2, 2)), jnp.float32)
    up_train = gaussian(key_list[3], (EXPERTS, D, FF), D ** -0.5, 0.125, ((1, 16), (2, 2)), jnp.float32)
    down_train = gaussian(key_list[4], (EXPERTS, FF, D), FF ** -0.5, 0.1875, ((1, 2), (2, 16)), jnp.float32)
    expert_ids_keys = jax.random.split(jax.random.fold_in(key_list[5], 1), TOKENS // TOK_DEV)
    expert_ids_turns = jax.random.permutation(jax.random.fold_in(key_list[5], 3), TOKENS // TOK_DEV)
    expert_ids = jax.vmap(lambda own, number: assign_block(jax.random.fold_in(key_list[5], 2), own, number, TOK_DEV, EXPERTS, 2, CAP, 2))(expert_ids_keys, expert_ids_turns).reshape((TOKENS, 2))
    route_score = jnp.clip(jnp.exp(math.log(1.0) - 2.9957323 * jax.random.uniform(key_list[6], (TOKENS, 2), jnp.float32) ** block_levels(key_list[6], (TOKENS, 2), ((0, 16),), -0.2, 0.2)), 0.05, 1.0)
    return dict(tokens=tokens, norm_gain=norm_gain, gate_train=gate_train, up_train=up_train, down_train=down_train, expert_ids=expert_ids, route_score=route_score)


epsilon = 1e-06

def reference(tokens, norm_gain, gate_train, up_train, down_train, expert_ids, route_score):
    gate_ready = (norm_gain[None, :, None] * gate_train).astype(jnp.bfloat16)
    up_ready = (norm_gain[None, :, None] * up_train).astype(jnp.bfloat16)
    down_ready = down_train.astype(jnp.bfloat16)
    floated = tokens.astype(jnp.float32)
    normed = (floated * lax.rsqrt(lax.optimization_barrier(jnp.mean(floated * floated, axis=-1, keepdims=True)) + epsilon)).astype(jnp.bfloat16)
    route_share = route_score / lax.optimization_barrier(jnp.sum(route_score, axis=-1, keepdims=True))
    blocks = N_GR * N_FS
    picks = TOK_DEV * 2
    flat_ids = expert_ids.reshape(blocks, picks)
    flat_share = route_share.reshape(blocks, picks)
    token_of = ((jnp.arange(picks, dtype=jnp.int32) // 2)[None, :] + (jnp.arange(blocks, dtype=jnp.int32) * TOK_DEV)[:, None]).astype(jnp.int32)
    block_rows = jnp.broadcast_to(jnp.arange(blocks, dtype=jnp.int32)[:, None], (blocks, picks))
    hidden_block = FF // N_TP

    def per_expert(total, expert):
        matches = (flat_ids == expert).astype(jnp.int32)
        ranked = jnp.cumsum(matches, axis=1) - 1
        column = jnp.where(matches > 0, ranked, CAP).astype(jnp.int32)
        token_table = jnp.zeros((blocks, CAP), jnp.int32).at[block_rows, column].set(token_of, mode='drop')
        share_table = jnp.zeros((blocks, CAP), jnp.float32).at[block_rows, column].set(flat_share, mode='drop')
        token_index = token_table.reshape(-1)
        picked_rows = normed[token_index]
        gate_act = jnp.dot(picked_rows, gate_ready[expert], preferred_element_type=jnp.float32)
        up_act = jnp.dot(picked_rows, up_ready[expert], preferred_element_type=jnp.float32)
        hidden = (jax.nn.silu(gate_act) * up_act).astype(jnp.bfloat16)
        partial_value = jnp.einsum('rnh,nhk->rnk', hidden.reshape(-1, N_TP, hidden_block).astype(jnp.float32), down_ready[expert].reshape(N_TP, hidden_block, D).astype(jnp.float32))
        rounded = lax.optimization_barrier(partial_value.astype(jnp.bfloat16))
        expert_out = lax.optimization_barrier(jnp.sum(rounded.astype(jnp.float32), axis=1)).astype(jnp.bfloat16)
        total = total.at[token_index].add(share_table.reshape(-1)[:, None] * expert_out.astype(jnp.float32))
        return (total, None)
    start = jnp.zeros((TOKENS, D), jnp.float32)
    summed, _ = lax.scan(per_expert, start, jnp.arange(EXPERTS, dtype=jnp.int32))
    return (gate_ready, up_ready, down_ready, summed.astype(jnp.bfloat16))
```

```python
import functools

import jax
import jax.numpy as jnp
from jax import lax
from jax.experimental import pallas as pl
from jax.experimental.pallas import tpu as pltpu
from jax.sharding import PartitionSpec as P

epsilon = 1e-06
MESH = pl.DeviceIdType.MESH


def remote(src, dst, send_sem, recv_sem, where):
    return pltpu.make_async_remote_copy(
        src_ref=src, dst_ref=dst, send_sem=send_sem, recv_sem=recv_sem, device_id=where, device_id_type=MESH
    )


def greet(sizes):
    barrier = pltpu.get_barrier_semaphore()
    count = 0
    for name, size in sizes.items():
        me = lax.axis_index(name)
        for k in range(1, size):
            pl.semaphore_signal(barrier, inc=1, device_id={name: lax.rem(me + k, size)}, device_id_type=MESH)
            count += 1
    pl.semaphore_wait(barrier, count)


def spread_kernel(sizes, local, direct_down, gate, up, down, rows, keys, gate_out, up_out, down_out, rows_out, keys_out,
                  w_send, w_recv, g_send, g_recv, up_send, low_send, y_send, x_recv, t_send, t_recv, k_send, k_recv, own_sem):
    n_gr, n_fs, n_tp = sizes["gr"], sizes["fs"], sizes["tp"]
    g, f, p = lax.axis_index("gr"), lax.axis_index("fs"), lax.axis_index("tp")
    inner = 2 if n_fs % 2 == 0 else 1
    lines = n_fs // inner
    z, y = f // inner, lax.rem(f, inner)
    depth = gate.shape[1]
    half = rows.shape[1] // n_tp
    cols = pl.ds(pl.multiple_of(p * half, half), half)
    sources, outs = (gate, up, down), (gate_out, up_out, down_out)

    def place(w, block):
        start = pl.multiple_of(block * depth, depth)
        if w < 2:
            return outs[w].at[:, pl.ds(start, depth), :]
        return outs[w].at[:, :, pl.ds(start, depth)] if direct_down else outs[w].at[block]

    greet(sizes)

    own = [pltpu.make_async_copy(rows, rows_out.at[f], own_sem.at[0]),
           pltpu.make_async_copy(keys, keys_out.at[f], own_sem.at[1])]
    for w in range(3):
        own.append(pltpu.make_async_copy(sources[w].at[pl.ds(f * local, local)], place(w, g * n_fs + f), own_sem.at[2 + w]))

    def block_of(b):
        return rows_out.at[b, :, cols]

    def row_copy(b, first, kind, where):
        src = rows.at[:, cols] if first else block_of(b)
        return remote(src, block_of(b), {"u": up_send, "d": low_send, "y": y_send}[kind].at[b], x_recv.at[b], where)

    def tp_copy(b, j):
        return remote(block_of(b), block_of(b), t_send.at[j, b], t_recv.at[j, b], {"tp": lax.rem(p + j + 1, n_tp)})

    def go_up(b, first, act):
        @pl.when(z < lines - 1)
        def _():
            act(row_copy(b, first, "u", {"fs": lax.rem(f + inner, n_fs)}))

    def go_down(b, first, act):
        @pl.when(z > 0)
        def _():
            act(row_copy(b, first, "d", {"fs": lax.rem(f + n_fs - inner, n_fs)}))

    def go_side(b, first, act):
        if inner == 2:
            act(row_copy(b, first, "y", {"fs": f + 1 - 2 * y}))

    def start(c):
        c.start()

    def recv(c):
        c.wait_recv()

    def sent(c):
        c.wait_send()

    go_up(f, True, start)
    go_down(f, True, start)
    go_side(f, True, start)
    key_copies = []
    for k in range(1, n_fs):
        to = lax.rem(f + k, n_fs)
        c = remote(keys, keys_out.at[f], k_send.at[k], k_recv.at[k], {"fs": to})
        c.start()
        key_copies.append(c)
    for c in own:
        c.start()

    def gr_copy(w, b, k, j, first):
        src = sources[w].at[pl.ds(f * local, local)] if first else place(w, b)
        return remote(src, place(w, b), g_send.at[w, k, j], g_recv.at[w, k, j], {"gr": lax.rem(g + j + 1, n_gr)})

    for w in range(3):
        for j in range(n_gr - 1):
            gr_copy(w, g * n_fs + f, 0, j, True).start()

    for s in range(1, lines):
        @pl.when(z >= s)
        def _():
            b = f - s * inner
            row_copy(b, False, "u", {"fs": lax.rem(f + inner, n_fs)}).wait_recv()
            go_up(b, False, start)
            go_side(b, False, start)
            for j in range(n_tp - 1):
                tp_copy(b, j).start()

        @pl.when(z < lines - s)
        def _():
            b = f + s * inner
            row_copy(b, False, "d", {"fs": lax.rem(f + inner, n_fs)}).wait_recv()
            go_down(b, False, start)
            go_side(b, False, start)
            for j in range(n_tp - 1):
                tp_copy(b, j).start()

    def w_copy(w, k):
        to = lax.rem(f + k, n_fs)
        return remote(sources[w].at[pl.ds(to * local, local)], place(w, g * n_fs + f), w_send.at[w, k], w_recv.at[w, k], {"fs": to})

    for w in range(3):
        for k in range(1, n_fs):
            w_copy(w, k).start()

    if inner == 2:
        for s in range(lines):
            b = lax.rem(z + s, lines) * inner + 1 - y
            row_copy(b, False, "y", {"fs": f + 1 - 2 * y}).wait_recv()
            for j in range(n_tp - 1):
                tp_copy(b, j).start()

    for w in range(3):
        for k in range(1, n_fs):
            w_copy(w, k).wait_recv()
            b = g * n_fs + lax.rem(f + n_fs - k, n_fs)
            for j in range(n_gr - 1):
                gr_copy(w, b, k, j, False).start()

    for k in range(1, n_fs):
        b = lax.rem(f + k, n_fs)
        for j in range(n_tp - 1):
            c = tp_copy(b, j)
            c.wait_recv()
            c.wait_send()
    for c in key_copies:
        c.wait_recv()
        c.wait_send()
    for c in own:
        c.wait()
    go_up(f, True, sent)
    go_down(f, True, sent)
    go_side(f, True, sent)
    for s in range(1, lines):
        @pl.when(z >= s)
        def _():
            go_up(f - s * inner, False, sent)
            go_side(f - s * inner, False, sent)

        @pl.when(z < lines - s)
        def _():
            go_down(f + s * inner, False, sent)
            go_side(f + s * inner, False, sent)
    for w in range(3):
        for k in range(n_fs):
            if k:
                w_copy(w, k).wait_send()
            for j in range(n_gr - 1):
                c = gr_copy(w, g * n_fs + lax.rem(f + n_fs - k, n_fs), k, j, False)
                c.wait_recv()
                c.wait_send()


def return_kernel(sizes, part, out, held, total, t_send, t_recv, f_send, f_recv):
    n_fs, n_tp = sizes["fs"], sizes["tp"]
    f, p = lax.axis_index("fs"), lax.axis_index("tp")
    half = part.shape[2] // n_tp

    def cols(q):
        return pl.ds(pl.multiple_of(q * half, half), half)

    greet({"fs": n_fs, "tp": n_tp})
    order = list(range(1, n_fs)) + [0]

    def tp_copy(k, j):
        to = lax.rem(p + j + 1, n_tp)
        b = lax.rem(f + k, n_fs)
        return remote(part.at[b, :, cols(to)], held.at[j, b], t_send.at[j, k], t_recv.at[j, k], {"tp": to})

    def f_copy(k):
        b = lax.rem(f + k, n_fs)
        return remote(total.at[b], out.at[f], f_send.at[k], f_recv.at[k], {"fs": b})

    for k in order:
        for j in range(n_tp - 1):
            tp_copy(k, j).start()
    for k in order:
        b = lax.rem(f + k, n_fs)
        value = part[b, :, cols(p)].astype(jnp.float32)
        for j in range(n_tp - 1):
            tp_copy(k, j).wait_recv()
            value = value + held[j, b].astype(jnp.float32)
        value = value.astype(jnp.bfloat16)
        if k == 0:
            out[b] = value
        else:
            total[b] = value
            f_copy(k).start()
    for k in order:
        for j in range(n_tp - 1):
            tp_copy(k, j).wait_send()
        if k:
            f_copy(k).wait_recv()
            f_copy(k).wait_send()


def on_device(sizes, tokens, norm_gain, gate_train, up_train, down_train, expert_ids, route_score):
    n_gr, n_fs, n_tp = sizes["gr"], sizes["fs"], sizes["tp"]
    bf16 = jnp.bfloat16
    experts, depth, hid = gate_train.shape
    local = experts // n_fs
    count, width = tokens.shape
    capacity = 4 * count // experts
    gate_cast = (norm_gain[None, :, None] * gate_train).astype(bf16)
    up_cast = (norm_gain[None, :, None] * up_train).astype(bf16)
    down_cast = down_train.astype(bf16)
    floated = tokens.astype(jnp.float32)
    normed = (floated * lax.rsqrt(jnp.mean(floated * floated, axis=-1, keepdims=True) + epsilon)).astype(bf16)

    named = expert_ids[:, :, None] == jnp.arange(experts, dtype=jnp.int32)
    names = jnp.any(named, axis=1)
    earlier = jnp.arange(count)[:, None] > jnp.arange(count)[None, :]
    rank = jnp.dot(earlier.astype(bf16), names.astype(bf16), preferred_element_type=jnp.float32).astype(jnp.int32)
    slot = expert_ids * capacity + jnp.sum(jnp.where(named, rank[:, None, :], 0), axis=2)
    keys = jnp.concatenate([slot.T, jnp.full((6, count), -1, jnp.int32)], axis=0)

    direct_down = depth % 128 == 0
    down_shape = (local, hid, n_gr * n_fs * depth) if direct_down else (n_gr * n_fs, local, hid, depth)
    dma = pltpu.SemaphoreType.DMA
    gate_ready, up_ready, down_ready, gathered, all_keys = pl.pallas_call(
        functools.partial(spread_kernel, sizes, local, direct_down),
        out_shape=(
            jax.ShapeDtypeStruct((local, n_gr * n_fs * depth, hid), bf16),
            jax.ShapeDtypeStruct((local, n_gr * n_fs * depth, hid), bf16),
            jax.ShapeDtypeStruct(down_shape, bf16),
            jax.ShapeDtypeStruct((n_fs, count, width), bf16),
            jax.ShapeDtypeStruct((n_fs, 8, count), jnp.int32),
        ),
        in_specs=[pl.BlockSpec(memory_space=pltpu.VMEM)] * 5,
        out_specs=[pl.BlockSpec(memory_space=pl.ANY)] * 5,
        scratch_shapes=[
            dma((3, n_fs)), dma((3, n_fs)), dma((3, n_fs, n_gr)), dma((3, n_fs, n_gr)),
            dma((n_fs,)), dma((n_fs,)), dma((n_fs,)), dma((n_fs,)),
            dma((n_tp, n_fs)), dma((n_tp, n_fs)), dma((n_fs,)), dma((n_fs,)), dma((5,)),
        ],
        compiler_params=pltpu.CompilerParams(collective_id=0, has_side_effects=True),
        name="spread",
    )(gate_cast, up_cast, down_cast, normed, keys)
    if not direct_down:
        down_ready = down_ready.transpose(1, 2, 0, 3).reshape(local, hid, -1)

    wanted = (lax.axis_index("fs") * local * capacity + jnp.arange(local * capacity, dtype=jnp.int32))[None, :, None]
    pick = ((all_keys[:, 0][:, None, :] == wanted) | (all_keys[:, 1][:, None, :] == wanted)).astype(bf16)
    rows = jnp.einsum("sct,std->scd", pick, gathered, preferred_element_type=jnp.float32).astype(bf16)
    rows = rows.reshape(n_fs, local, capacity, width)
    gate_act = jnp.einsum("seck,ekh->sech", rows, gate_ready, preferred_element_type=jnp.float32)
    up_act = jnp.einsum("seck,ekh->sech", rows, up_ready, preferred_element_type=jnp.float32)
    hidden = (jax.nn.silu(gate_act) * up_act).astype(bf16)
    part = jnp.einsum("sech,ehk->seck", hidden, down_ready, preferred_element_type=jnp.float32).astype(bf16)
    part = part.reshape(n_fs, local * capacity, width)
    half = width // n_tp
    returned = pl.pallas_call(
        functools.partial(return_kernel, sizes),
        out_shape=jax.ShapeDtypeStruct((n_fs, local * capacity, half), bf16),
        in_specs=[pl.BlockSpec(memory_space=pltpu.VMEM)],
        out_specs=pl.BlockSpec(memory_space=pltpu.VMEM),
        scratch_shapes=[
            pltpu.VMEM((max(n_tp - 1, 1), n_fs, local * capacity, half), bf16),
            pltpu.VMEM((n_fs, local * capacity, half), bf16),
            dma((n_tp, n_fs)), dma((n_tp, n_fs)), dma((n_fs,)), dma((n_fs,)),
        ],
        compiler_params=pltpu.CompilerParams(collective_id=1, has_side_effects=True),
        name="giveback",
    )(part)
    share = route_score / jnp.sum(route_score, axis=-1, keepdims=True)
    at = jnp.arange(experts * capacity, dtype=jnp.int32)[None, :]
    weight = jnp.where(slot[:, :1] == at, share[:, :1], 0.0) + jnp.where(slot[:, 1:] == at, share[:, 1:], 0.0)
    mixed = jnp.dot(weight.astype(bf16), returned.reshape(experts * capacity, half), preferred_element_type=jnp.float32)
    return gate_ready, up_ready, down_ready, mixed.astype(bf16)


def solution(mesh):
    return jax.shard_map(
        functools.partial(on_device, dict(mesh.shape)),
        mesh=mesh,
        in_specs=(
            P(("gr", "fs"), None),
            P(("gr", "fs")),
            P(None, ("gr", "fs"), "tp"),
            P(None, ("gr", "fs"), "tp"),
            P(None, "tp", ("gr", "fs")),
            P(("gr", "fs"), None),
            P(("gr", "fs"), None),
        ),
        out_specs=(
            P("fs", None, "tp"),
            P("fs", None, "tp"),
            P("fs", "tp", None),
            P(("gr", "fs"), "tp"),
        ),
        check_vma=False,
    )
```

```python
import functools

import jax
import jax.numpy as jnp
from jax import lax
from jax.experimental import pallas as pl
from jax.experimental.pallas import tpu as pltpu
from jax.sharding import PartitionSpec as P

epsilon = 1e-06
MESH = pl.DeviceIdType.MESH


def remote(src, dst, send_sem, recv_sem, where):
    return pltpu.make_async_remote_copy(
        src_ref=src, dst_ref=dst, send_sem=send_sem, recv_sem=recv_sem, device_id=where, device_id_type=MESH
    )


def greet(sizes):
    barrier = pltpu.get_barrier_semaphore()
    count = 0
    for name, size in sizes.items():
        me = lax.axis_index(name)
        for k in range(1, size):
            pl.semaphore_signal(barrier, inc=1, device_id={name: lax.rem(me + k, size)}, device_id_type=MESH)
            count += 1
    pl.semaphore_wait(barrier, count)


def spread_kernel(sizes, local, direct_down, gate, up, down, rows, keys, gate_out, up_out, down_out, rows_out, keys_out,
                  w_send, w_recv, g_send, g_recv, up_send, low_send, y_send, x_recv, t_send, t_recv, k_send, k_recv, own_sem):
    n_gr, n_fs, n_tp = sizes["gr"], sizes["fs"], sizes["tp"]
    g, f, p = lax.axis_index("gr"), lax.axis_index("fs"), lax.axis_index("tp")
    inner = 2 if n_fs % 2 == 0 else 1
    lines = n_fs // inner
    z, y = f // inner, lax.rem(f, inner)
    depth = gate.shape[1]
    half = rows.shape[1] // n_tp
    cols = pl.ds(pl.multiple_of(p * half, half), half)
    sources, outs = (gate, up, down), (gate_out, up_out, down_out)

    def place(w, block):
        start = pl.multiple_of(block * depth, depth)
        if w < 2:
            return outs[w].at[:, pl.ds(start, depth), :]
        return outs[w].at[:, :, pl.ds(start, depth)] if direct_down else outs[w].at[block]

    greet(sizes)

    own = [pltpu.make_async_copy(rows, rows_out.at[f], own_sem.at[0]),
           pltpu.make_async_copy(keys, keys_out.at[f], own_sem.at[1])]
    for w in range(3):
        own.append(pltpu.make_async_copy(sources[w].at[pl.ds(f * local, local)], place(w, g * n_fs + f), own_sem.at[2 + w]))

    def block_of(b):
        return rows_out.at[b, :, cols]

    def row_copy(b, first, kind, where):
        src = rows.at[:, cols] if first else block_of(b)
        return remote(src, block_of(b), {"u": up_send, "d": low_send, "y": y_send}[kind].at[b], x_recv.at[b], where)

    def tp_copy(b, j):
        return remote(block_of(b), block_of(b), t_send.at[j, b], t_recv.at[j, b], {"tp": lax.rem(p + j + 1, n_tp)})

    def go_up(b, first, act):
        @pl.when(z < lines - 1)
        def _():
            act(row_copy(b, first, "u", {"fs": lax.rem(f + inner, n_fs)}))

    def go_down(b, first, act):
        @pl.when(z > 0)
        def _():
            act(row_copy(b, first, "d", {"fs": lax.rem(f + n_fs - inner, n_fs)}))

    def go_side(b, first, act):
        if inner == 2:
            act(row_copy(b, first, "y", {"fs": f + 1 - 2 * y}))

    def start(c):
        c.start()

    def recv(c):
        c.wait_recv()

    def sent(c):
        c.wait_send()

    go_up(f, True, start)
    go_down(f, True, start)
    go_side(f, True, start)
    key_copies = []
    for k in range(1, n_fs):
        to = lax.rem(f + k, n_fs)
        c = remote(keys, keys_out.at[f], k_send.at[k], k_recv.at[k], {"fs": to})
        c.start()
        key_copies.append(c)
    for c in own:
        c.start()

    def gr_copy(w, b, k, j, first):
        src = sources[w].at[pl.ds(f * local, local)] if first else place(w, b)
        return remote(src, place(w, b), g_send.at[w, k, j], g_recv.at[w, k, j], {"gr": lax.rem(g + j + 1, n_gr)})

    for w in range(3):
        for j in range(n_gr - 1):
            gr_copy(w, g * n_fs + f, 0, j, True).start()

    for s in range(1, lines):
        @pl.when(z >= s)
        def _():
            b = f - s * inner
            row_copy(b, False, "u", {"fs": lax.rem(f + inner, n_fs)}).wait_recv()
            go_up(b, False, start)
            go_side(b, False, start)
            for j in range(n_tp - 1):
                tp_copy(b, j).start()

        @pl.when(z < lines - s)
        def _():
            b = f + s * inner
            row_copy(b, False, "d", {"fs": lax.rem(f + inner, n_fs)}).wait_recv()
            go_down(b, False, start)
            go_side(b, False, start)
            for j in range(n_tp - 1):
                tp_copy(b, j).start()

    def w_copy(w, k):
        to = lax.rem(f + k, n_fs)
        return remote(sources[w].at[pl.ds(to * local, local)], place(w, g * n_fs + f), w_send.at[w, k], w_recv.at[w, k], {"fs": to})

    for w in range(3):
        for k in range(1, n_fs):
            w_copy(w, k).start()

    if inner == 2:
        for s in range(lines):
            b = lax.rem(z + s, lines) * inner + 1 - y
            row_copy(b, False, "y", {"fs": f + 1 - 2 * y}).wait_recv()
            for j in range(n_tp - 1):
                tp_copy(b, j).start()

    for w in range(3):
        for k in range(1, n_fs):
            w_copy(w, k).wait_recv()
            b = g * n_fs + lax.rem(f + n_fs - k, n_fs)
            for j in range(n_gr - 1):
                gr_copy(w, b, k, j, False).start()

    for k in range(1, n_fs):
        b = lax.rem(f + k, n_fs)
        for j in range(n_tp - 1):
            c = tp_copy(b, j)
            c.wait_recv()
            c.wait_send()
    for c in key_copies:
        c.wait_recv()
        c.wait_send()
    for c in own:
        c.wait()
    go_up(f, True, sent)
    go_down(f, True, sent)
    go_side(f, True, sent)
    for s in range(1, lines):
        @pl.when(z >= s)
        def _():
            go_up(f - s * inner, False, sent)
            go_side(f - s * inner, False, sent)

        @pl.when(z < lines - s)
        def _():
            go_down(f + s * inner, False, sent)
            go_side(f + s * inner, False, sent)
    for w in range(3):
        for k in range(n_fs):
            if k:
                w_copy(w, k).wait_send()
            for j in range(n_gr - 1):
                c = gr_copy(w, g * n_fs + lax.rem(f + n_fs - k, n_fs), k, j, False)
                c.wait_recv()
                c.wait_send()


def return_kernel(sizes, part, out, held, total, t_send, t_recv, f_send, f_recv):
    n_fs, n_tp = sizes["fs"], sizes["tp"]
    f, p = lax.axis_index("fs"), lax.axis_index("tp")
    half = part.shape[2] // n_tp

    def cols(q):
        return pl.ds(pl.multiple_of(q * half, half), half)

    greet({"fs": n_fs, "tp": n_tp})
    order = list(range(1, n_fs)) + [0]

    def tp_copy(k, j):
        to = lax.rem(p + j + 1, n_tp)
        b = lax.rem(f + k, n_fs)
        return remote(part.at[b, :, cols(to)], held.at[j, b], t_send.at[j, k], t_recv.at[j, k], {"tp": to})

    def f_copy(k):
        b = lax.rem(f + k, n_fs)
        return remote(total.at[b], out.at[f], f_send.at[k], f_recv.at[k], {"fs": b})

    for k in order:
        for j in range(n_tp - 1):
            tp_copy(k, j).start()
    for k in order:
        b = lax.rem(f + k, n_fs)
        value = part[b, :, cols(p)].astype(jnp.float32)
        for j in range(n_tp - 1):
            tp_copy(k, j).wait_recv()
            value = value + held[j, b].astype(jnp.float32)
        value = value.astype(jnp.bfloat16)
        if k == 0:
            out[b] = value
        else:
            total[b] = value
            f_copy(k).start()
    for k in order:
        for j in range(n_tp - 1):
            tp_copy(k, j).wait_send()
        if k:
            f_copy(k).wait_recv()
            f_copy(k).wait_send()


def fused_kernel(sizes, gate, up, down, rows, keys, weight, gate_hbm, up_hbm, down_hbm, mixed,
                 gate_in, up_in, down_in, rows_in, keys_in, picked, hidden, part, held, total, back, acc,
                 w_send, w_recv, g_send, g_recv, up_send, low_send, y_send, x_recv, t_send, t_recv, k_send, k_recv,
                 p_send, p_recv, f_send, f_recv, own_sem, out_sem):
    n_gr, n_fs, n_tp = sizes["gr"], sizes["fs"], sizes["tp"]
    g, f, p = lax.axis_index("gr"), lax.axis_index("fs"), lax.axis_index("tp")
    inner = 2 if n_fs % 2 == 0 else 1
    lines = n_fs // inner
    z, y = f // inner, lax.rem(f, inner)
    depth = gate.shape[1]
    count, width = rows.shape
    slots = weight.shape[2]
    half = width // n_tp
    bf16, f32 = jnp.bfloat16, jnp.float32
    sources, outs, finals = (gate, up, down), (gate_in, up_in, down_in), (gate_hbm, up_hbm, down_hbm)

    def cols(q):
        return pl.ds(pl.multiple_of(q * half, half), half)

    def near(k):
        return lax.rem(f + k, n_fs)

    def place(w, block):
        span = pl.ds(pl.multiple_of(block * depth, depth), depth)
        return outs[w].at[span, :] if w < 2 else outs[w].at[:, span]

    above, below, beside = {"fs": near(inner)}, {"fs": near(n_fs - inner)}, {"fs": f + 1 - 2 * y}

    def block_of(b):
        return rows_in.at[b, :, cols(p)]

    def row_copy(b, first, sems, where):
        return remote(rows.at[:, cols(p)] if first else block_of(b), block_of(b), sems.at[b], x_recv.at[b], where)

    def tp_copy(b, j):
        return remote(block_of(b), block_of(b), t_send.at[j, b], t_recv.at[j, b], {"tp": lax.rem(p + j + 1, n_tp)})

    def go_up(b, first, act):
        @pl.when(z < lines - 1)
        def _():
            act(row_copy(b, first, up_send, above))

    def go_down(b, first, act):
        @pl.when(z > 0)
        def _():
            act(row_copy(b, first, low_send, below))

    def go_side(b, first, act):
        if inner == 2:
            act(row_copy(b, first, y_send, beside))

    def start(c):
        c.start()

    def sent(c):
        c.wait_send()

    def gr_copy(w, k, j):
        src = sources[w].at[f] if k == 0 else place(w, g * n_fs + near(n_fs - k))
        return remote(src, place(w, g * n_fs + near(n_fs - k)), g_send.at[w, k, j], g_recv.at[w, k, j],
                      {"gr": lax.rem(g + j + 1, n_gr)})

    def w_copy(w, k):
        to = near(k)
        return remote(sources[w].at[to], place(w, g * n_fs + f), w_send.at[w, k], w_recv.at[w, k], {"fs": to})

    def send_weights(w):
        for k in range(1, n_fs):
            w_copy(w, k).start()

    def pass_on(w, k):
        w_copy(w, k).wait_recv()
        for j in range(n_gr - 1):
            gr_copy(w, k, j).start()

    def line_step(s):
        @pl.when(z >= s)
        def _():
            b = f - s * inner
            row_copy(b, False, up_send, above).wait_recv()
            go_up(b, False, start)
            go_side(b, False, start)
            for j in range(n_tp - 1):
                tp_copy(b, j).start()

        @pl.when(z < lines - s)
        def _():
            b = f + s * inner
            row_copy(b, False, low_send, below).wait_recv()
            go_down(b, False, start)
            go_side(b, False, start)
            for j in range(n_tp - 1):
                tp_copy(b, j).start()

    def whole(w):
        for k in range(n_fs):
            for j in range(n_gr - 1):
                gr_copy(w, k, j).wait_recv()
        pltpu.make_async_copy(outs[w], finals[w].at[0], out_sem.at[w]).start()

    def pick_rows(b):
        table = keys_in[b]
        wanted = f * slots + lax.broadcasted_iota(jnp.int32, (slots, count), 0)
        hit = ((table[0:1, :] == wanted) | (table[1:2, :] == wanted)).astype(f32).astype(bf16)
        for c in range(0, width, 512):
            picked[pl.ds(pl.multiple_of(b * slots, slots), slots), c:c + 512] = jnp.dot(
                hit, rows_in[b, :, c:c + 512], preferred_element_type=f32).astype(bf16)

    greet(sizes)

    own = [pltpu.make_async_copy(rows, rows_in.at[f], own_sem.at[0]),
           pltpu.make_async_copy(keys, keys_in.at[f], own_sem.at[1])]
    for w in range(3):
        own.append(pltpu.make_async_copy(sources[w].at[f], place(w, g * n_fs + f), own_sem.at[2 + w]))

    def key_copy(k):
        return remote(keys, keys_in.at[f], k_send.at[k], k_recv.at[k], {"fs": near(k)})

    go_up(f, True, start)
    go_down(f, True, start)
    go_side(f, True, start)
    for k in range(1, n_fs):
        key_copy(k).start()
    for c in own:
        c.start()
    for w in range(3):
        for j in range(n_gr - 1):
            gr_copy(w, 0, j).start()
    send_weights(0)
    if lines > 1:
        line_step(1)
    send_weights(1)
    for k in range(1, n_fs):
        pass_on(0, k)
    if lines > 2:
        line_step(2)
    send_weights(2)
    for s in range(3, lines):
        line_step(s)
    if inner == 2:
        for s in range(lines):
            b = lax.rem(z + s, lines) * inner + 1 - y
            row_copy(b, False, y_send, beside).wait_recv()
            for j in range(n_tp - 1):
                tp_copy(b, j).start()
    for c in own:
        c.wait()
    pick_rows(f)
    for k in range(1, n_fs):
        pass_on(1, k)
        b = near(n_fs - k)
        for j in range(n_tp - 1):
            tp_copy(b, j).wait_recv()
        key_copy(k).wait_recv()
        pick_rows(b)
    whole(0)
    whole(1)
    group = 2 if n_fs % 2 == 0 else 1
    for i in range(n_fs // group):
        for k in range(1 + i * group, min(1 + (i + 1) * group, n_fs)):
            pass_on(2, k)
        span = slice(i * group * slots, (i + 1) * group * slots)
        gate_act = jnp.dot(picked[span, :], gate_in[...], preferred_element_type=f32)
        up_act = jnp.dot(picked[span, :], up_in[...], preferred_element_type=f32)
        hidden[span, :] = (gate_act / (1.0 + jnp.exp(-gate_act)) * up_act).astype(bf16)
    whole(2)

    order = list(range(1, n_fs)) + [0]

    def p_copy(k, j):
        to = lax.rem(p + j + 1, n_tp)
        b = near(k)
        return remote(part.at[b, :, cols(to)], held.at[j, b], p_send.at[j, k], p_recv.at[j, k], {"tp": to})

    def f_copy(k):
        return remote(total.at[near(k)], back.at[f], f_send.at[k], f_recv.at[k], {"fs": near(k)})

    for i in range(n_fs + 3):
        if i < n_fs:
            b = near(order[i])
            mine = hidden[pl.ds(pl.multiple_of(b * slots, slots), slots), :]
            for c in range(0, width, 512):
                part[b, :, c:c + 512] = jnp.dot(mine, down_in[:, c:c + 512], preferred_element_type=f32).astype(bf16)
        if 0 <= i - 1 < n_fs:
            for j in range(n_tp - 1):
                p_copy(order[i - 1], j).start()
        if 0 <= i - 2 < n_fs:
            k = order[i - 2]
            b = near(k)
            value = part[b, :, cols(p)].astype(f32)
            for j in range(n_tp - 1):
                p_copy(k, j).wait_recv()
                value = value + held[j, b].astype(f32)
            total[b] = value.astype(bf16)
        if 0 <= i - 3 < n_fs and order[i - 3]:
            f_copy(order[i - 3]).start()

    acc[...] = jnp.dot(weight[f], total[f], preferred_element_type=f32)
    for k in range(1, n_fs):
        f_copy(k).wait_recv()
        b = near(n_fs - k)
        acc[...] += jnp.dot(weight[b], back[b], preferred_element_type=f32)
    mixed[...] = acc[...].astype(bf16)

    for k in range(n_fs):
        for j in range(n_tp - 1):
            p_copy(k, j).wait_send()
        if k:
            f_copy(k).wait_send()
            key_copy(k).wait_send()
            for j in range(n_tp - 1):
                tp_copy(near(k), j).wait_send()
        for w in range(3):
            if k:
                w_copy(w, k).wait_send()
            for j in range(n_gr - 1):
                gr_copy(w, k, j).wait_send()
    go_up(f, True, sent)
    go_down(f, True, sent)
    go_side(f, True, sent)
    for s in range(1, lines):
        @pl.when(z >= s)
        def _():
            go_up(f - s * inner, False, sent)
            go_side(f - s * inner, False, sent)

        @pl.when(z < lines - s)
        def _():
            go_down(f + s * inner, False, sent)
            go_side(f + s * inner, False, sent)
    for w in range(3):
        pltpu.make_async_copy(outs[w], finals[w].at[0], out_sem.at[w]).wait()


def run_fused(sizes, gate_cast, up_cast, down_cast, normed, keys, weight):
    n_gr, n_fs, n_tp = sizes["gr"], sizes["fs"], sizes["tp"]
    _, depth, hid = gate_cast.shape
    count, width = normed.shape
    slots = weight.shape[2]
    half = width // n_tp
    bf16, dma = jnp.bfloat16, pltpu.SemaphoreType.DMA
    vmem = pl.BlockSpec(memory_space=pltpu.VMEM)
    return pl.pallas_call(
        functools.partial(fused_kernel, sizes),
        out_shape=(
            jax.ShapeDtypeStruct((1, n_gr * n_fs * depth, hid), bf16),
            jax.ShapeDtypeStruct((1, n_gr * n_fs * depth, hid), bf16),
            jax.ShapeDtypeStruct((1, hid, n_gr * n_fs * depth), bf16),
            jax.ShapeDtypeStruct((count, half), bf16),
        ),
        in_specs=[vmem] * 6,
        out_specs=[pl.BlockSpec(memory_space=pl.ANY)] * 3 + [vmem],
        scratch_shapes=[
            pltpu.VMEM((n_gr * n_fs * depth, hid), bf16), pltpu.VMEM((n_gr * n_fs * depth, hid), bf16),
            pltpu.VMEM((hid, n_gr * n_fs * depth), bf16),
            pltpu.VMEM((n_fs, count, width), bf16), pltpu.VMEM((n_fs, 8, count), jnp.int32),
            pltpu.VMEM((n_fs * slots, width), bf16), pltpu.VMEM((n_fs * slots, hid), bf16),
            pltpu.VMEM((n_fs, slots, width), bf16),
            pltpu.VMEM((max(n_tp - 1, 1), n_fs, slots, half), bf16),
            pltpu.VMEM((n_fs, slots, half), bf16), pltpu.VMEM((n_fs, slots, half), bf16),
            pltpu.VMEM((count, half), jnp.float32),
            dma((3, n_fs)), dma((3, n_fs)), dma((3, n_fs, n_gr)), dma((3, n_fs, n_gr)),
            dma((n_fs,)), dma((n_fs,)), dma((n_fs,)), dma((n_fs,)),
            dma((n_tp, n_fs)), dma((n_tp, n_fs)), dma((n_fs,)), dma((n_fs,)),
            dma((n_tp, n_fs)), dma((n_tp, n_fs)), dma((n_fs,)), dma((n_fs,)), dma((5,)), dma((3,)),
        ],
        compiler_params=pltpu.CompilerParams(collective_id=2, has_side_effects=True, vmem_limit_bytes=62 * 2**20),
        name="handover",
    )(gate_cast, up_cast, down_cast, normed, keys, weight)


def on_device(sizes, tokens, norm_gain, gate_train, up_train, down_train, expert_ids, route_score):
    n_gr, n_fs, n_tp = sizes["gr"], sizes["fs"], sizes["tp"]
    bf16 = jnp.bfloat16
    experts, depth, hid = gate_train.shape
    local = experts // n_fs
    count, width = tokens.shape
    capacity = 4 * count // experts
    gate_cast = (norm_gain[None, :, None] * gate_train).astype(bf16)
    up_cast = (norm_gain[None, :, None] * up_train).astype(bf16)
    down_cast = down_train.astype(bf16)
    floated = tokens.astype(jnp.float32)
    normed = (floated * lax.rsqrt(jnp.mean(floated * floated, axis=-1, keepdims=True) + epsilon)).astype(bf16)

    named = expert_ids[:, :, None] == jnp.arange(experts, dtype=jnp.int32)
    names = jnp.any(named, axis=1)
    earlier = jnp.arange(count)[:, None] > jnp.arange(count)[None, :]
    rank = jnp.dot(earlier.astype(bf16), names.astype(bf16), preferred_element_type=jnp.float32).astype(jnp.int32)
    slot = expert_ids * capacity + jnp.sum(jnp.where(named, rank[:, None, :], 0), axis=2)
    keys = jnp.concatenate([slot.T, jnp.full((6, count), -1, jnp.int32)], axis=0)

    share = route_score / jnp.sum(route_score, axis=-1, keepdims=True)
    direct_down = depth % 128 == 0
    if direct_down and local == 1 and capacity % 128 == 0:
        at = (jnp.arange(experts, dtype=jnp.int32)[:, None] * capacity + jnp.arange(capacity, dtype=jnp.int32))[:, None, :]
        weight = jnp.where(slot[None, :, :1] == at, share[None, :, :1], 0.0) + jnp.where(slot[None, :, 1:] == at, share[None, :, 1:], 0.0)
        return run_fused(sizes, gate_cast, up_cast, down_cast, normed, keys, weight.astype(bf16))

    down_shape = (local, hid, n_gr * n_fs * depth) if direct_down else (n_gr * n_fs, local, hid, depth)
    dma = pltpu.SemaphoreType.DMA
    gate_ready, up_ready, down_ready, gathered, all_keys = pl.pallas_call(
        functools.partial(spread_kernel, sizes, local, direct_down),
        out_shape=(
            jax.ShapeDtypeStruct((local, n_gr * n_fs * depth, hid), bf16),
            jax.ShapeDtypeStruct((local, n_gr * n_fs * depth, hid), bf16),
            jax.ShapeDtypeStruct(down_shape, bf16),
            jax.ShapeDtypeStruct((n_fs, count, width), bf16),
            jax.ShapeDtypeStruct((n_fs, 8, count), jnp.int32),
        ),
        in_specs=[pl.BlockSpec(memory_space=pltpu.VMEM)] * 5,
        out_specs=[pl.BlockSpec(memory_space=pl.ANY)] * 5,
        scratch_shapes=[
            dma((3, n_fs)), dma((3, n_fs)), dma((3, n_fs, n_gr)), dma((3, n_fs, n_gr)),
            dma((n_fs,)), dma((n_fs,)), dma((n_fs,)), dma((n_fs,)),
            dma((n_tp, n_fs)), dma((n_tp, n_fs)), dma((n_fs,)), dma((n_fs,)), dma((5,)),
        ],
        compiler_params=pltpu.CompilerParams(collective_id=0, has_side_effects=True),
        name="spread",
    )(gate_cast, up_cast, down_cast, normed, keys)
    if not direct_down:
        down_ready = down_ready.transpose(1, 2, 0, 3).reshape(local, hid, -1)

    wanted = (lax.axis_index("fs") * local * capacity + jnp.arange(local * capacity, dtype=jnp.int32))[None, :, None]
    pick = ((all_keys[:, 0][:, None, :] == wanted) | (all_keys[:, 1][:, None, :] == wanted)).astype(bf16)
    rows = jnp.einsum("sct,std->scd", pick, gathered, preferred_element_type=jnp.float32).astype(bf16)
    rows = rows.reshape(n_fs, local, capacity, width)
    gate_act = jnp.einsum("seck,ekh->sech", rows, gate_ready, preferred_element_type=jnp.float32)
    up_act = jnp.einsum("seck,ekh->sech", rows, up_ready, preferred_element_type=jnp.float32)
    hidden = (jax.nn.silu(gate_act) * up_act).astype(bf16)
    part = jnp.einsum("sech,ehk->seck", hidden, down_ready, preferred_element_type=jnp.float32).astype(bf16)
    part = part.reshape(n_fs, local * capacity, width)
    half = width // n_tp
    returned = pl.pallas_call(
        functools.partial(return_kernel, sizes),
        out_shape=jax.ShapeDtypeStruct((n_fs, local * capacity, half), bf16),
        in_specs=[pl.BlockSpec(memory_space=pltpu.VMEM)],
        out_specs=pl.BlockSpec(memory_space=pltpu.VMEM),
        scratch_shapes=[
            pltpu.VMEM((max(n_tp - 1, 1), n_fs, local * capacity, half), bf16),
            pltpu.VMEM((n_fs, local * capacity, half), bf16),
            dma((n_tp, n_fs)), dma((n_tp, n_fs)), dma((n_fs,)), dma((n_fs,)),
        ],
        compiler_params=pltpu.CompilerParams(collective_id=1, has_side_effects=True),
        name="giveback",
    )(part)
    at = jnp.arange(experts * capacity, dtype=jnp.int32)[None, :]
    weight = jnp.where(slot[:, :1] == at, share[:, :1], 0.0) + jnp.where(slot[:, 1:] == at, share[:, 1:], 0.0)
    mixed = jnp.dot(weight.astype(bf16), returned.reshape(experts * capacity, half), preferred_element_type=jnp.float32)
    return gate_ready, up_ready, down_ready, mixed.astype(bf16)


def solution(mesh):
    return jax.shard_map(
        functools.partial(on_device, dict(mesh.shape)),
        mesh=mesh,
        in_specs=(
            P(("gr", "fs"), None),
            P(("gr", "fs")),
            P(None, ("gr", "fs"), "tp"),
            P(None, ("gr", "fs"), "tp"),
            P(None, "tp", ("gr", "fs")),
            P(("gr", "fs"), None),
            P(("gr", "fs"), None),
        ),
        out_specs=(
            P("fs", None, "tp"),
            P("fs", None, "tp"),
            P("fs", "tp", None),
            P(("gr", "fs"), "tp"),
        ),
        check_vma=False,
    )
```
